32 devices in a mesh: ep: 8 (over z, y), tp: 4 (over x, core).
Axes of the slice: x: 2, y: 2, z: 4, core: 2. Of those that a mesh axis runs over, the one named last changes fastest.
Arguments:
- tokens: bfloat16 [1024, 2048], P('ep'), may hold values from -6 to 6
- norm_gain: float32 [2048], replicated, may hold values from 0.1 to 1.9
- routes: int32 [1024, 2], P('ep'), may hold values from 0 to 7, all different within a row; in each aligned block of 128 rows (0 to 127, 128 to 255, ...) at most 48 rows name the same one
- group_prob: float32 [1024], P('ep'), may hold values from 0.2 to 1
- expert_logits: float32 [1024, 2], P('ep'), may hold values from -6 to 6
- gate_weight: bfloat16 [8, 2048, 384], P('ep', None, 'tp'), may hold values from -0.125 to 0.125
- up_weight: bfloat16 [8, 2048, 384], P('ep', None, 'tp'), may hold values from -0.125 to 0.125
- down_matrix: bfloat16 [8, 384, 2048], P('ep', 'tp'), may hold values from -0.3125 to 0.3125
Outputs:
- combined: bfloat16 [1024, 2048], P('ep', 'tp')
The draws below stay inside these ranges and needn't reach their ends.
Inputs may be any that keep to these rules, and one draw needn't show every extreme that they name: `routes`: each row names 2 different experts. Among the 128 tokens of one index of ep at most 48 rows name one expert, and in every draw some expert is named by exactly 48 of them.
All inputs are finite; a program needn't handle non-finite values.
Results may differ from the reference program's by a relative error of at most 0.013.
Values may be sent and summed in bfloat16 or wider, within the bound.
A program may use at most 64 MiB of HBM per device.

```python
import math
import jax
import jax.numpy as jnp
import numpy as np
from jax import lax

MODEL_DIM = 2048
FF = 384
TOPK = 2
TOK_DEV = 128
EXPERTS = 8
CAP = 48
TOKENS = 1024
N_EP = 8
N_TP = 4


def shard_levels(key, shape, split, least, high):
    level, own = 1.0, jax.random.fold_in(key, 6)
    for axis_at, shards_of in split:
        draws = jnp.exp(jax.random.uniform(jax.random.fold_in(own, axis_at), (shards_of,), jnp.float32, least / len(split), high / len(split)))
        level = level * jnp.repeat(draws, shape[axis_at] // shards_of).reshape([-1 if axis == axis_at else 1 for axis in range(len(shape))])
    return level


def assign_block(stream_key, own, number, rows, number_of, top, limit, lean):
    sequence = jax.random.permutation(stream_key, number_of)
    heavy_load, common = shares(number_of, rows * top, limit, lean, True), shares(number_of, rows * top, limit, lean, False)
    places = jnp.arange(number_of)

    def named(lengths, turn):
        used = int((lengths > 0).sum())
        fixed = max(1, used // 4)
        passed = fixed + (places - fixed + turn * (used - fixed)) % max(1, number_of - fixed)
        return jnp.zeros((number_of,), jnp.int32).at[sequence[jnp.where(places < fixed, places, passed)]].set(jnp.asarray(lengths, jnp.int32))

    lengths = jnp.where(number % 4 == 0, named(heavy_load, number // 4), named(common, number - number // 4 - 1))
    mixed = jax.random.permutation(jax.random.fold_in(own, 3), number_of)
    giver, receiver = mixed[0:number_of // 2 * 2:2], mixed[1:number_of // 2 * 2:2]
    room = jnp.minimum(lengths[giver] - 1, limit - lengths[receiver]) // 2
    room = jnp.where((giver == sequence[0]) | (receiver == sequence[0]) | (lengths[receiver] == 0), 0, jnp.maximum(room, 0))
    passed = jax.random.randint(jax.random.fold_in(own, 4), (number_of // 2,), 0, 1 << 20) % (room + 1)
    lengths = lengths.at[giver].add(-passed).at[receiver].add(passed)
    labels = jnp.searchsorted(jnp.cumsum(lengths), jnp.arange(rows * top), side="right").astype(jnp.int32)
    listing = labels.reshape(top, rows).T
    listing = listing[jax.random.permutation(jax.random.fold_in(own, 1), rows)]
    turn = jax.random.randint(jax.random.fold_in(own, 2), (rows, 1), 0, top)
    return jnp.take_along_axis(listing, (jnp.arange(top)[None, :] + turn) % top, axis=1)


def shares(amount, total, limit, skew, full):
    portions = [(1 << 20) // math.isqrt(standing ** skew) + 1 for standing in range(1, amount + 1)]
    largest = limit if full else min(limit, max(-(-total // amount), total * portions[0] // sum(portions)))
    least = 1 if total - largest >= amount - 1 else 0
    holding, surplus = [largest] + [least] * (amount - 1), total - largest - least * (amount - 1)
    while surplus > 0:
        movable = [i for i in range(1, amount) if holding[i] < largest] or [i for i in range(1, amount) if holding[i] < limit]
        whole, remaining = sum([portions[i] for i in movable]), surplus
        for i in movable:
            extra = min(limit - holding[i], max(1, remaining * portions[i] // whole), surplus)
            holding[i] = holding[i] + extra
            surplus = surplus - extra
    return np.array(holding)


def bell_draw(rng, dims, spread, bound, shards=(), held_as=jnp.bfloat16):
    drawn = spread * jax.random.normal(rng, dims, jnp.float32)
    if shards:
        drawn = drawn * shard_levels(rng, dims, shards, -0.22, 0.18)
    return jnp.clip(drawn, -bound, bound).astype(held_as)


def setup_inputs(seed: int = 0) -> dict:
    key_of = jax.random.split(jax.random.key(seed), 9)
    tokens = bell_draw(key_of[0], (TOKENS, MODEL_DIM), 1.0, 6.0, ((0, 8),))
    norm_gain = jnp.clip(1.0 + 0.18 * jax.random.normal(key_of[1], (MODEL_DIM,), jnp.float32), 0.1, 1.9)
    routes_keys = jax.random.split(jax.random.fold_in(key_of[2], 1), TOKENS // TOK_DEV)
    routes_turns = jax.random.permutation(jax.random.fold_in(key_of[2], 3), TOKENS // TOK_DEV)
    routes = jax.vmap(lambda own, number: assign_block(jax.random.fold_in(key_of[2], 2), own, number, TOK_DEV, EXPERTS, TOPK, CAP, 2))(routes_keys, routes_turns).reshape((TOKENS, TOPK))
    group_prob = jnp.clip(0.2 + 0.8 * jax.random.uniform(key_of[3], (TOKENS,), jnp.float32) ** shard_levels(key_of[3], (TOKENS,), ((0, 8),), -0.2, 0.2), 0.2, 1.0)
    expert_logits = bell_draw(key_of[4], (TOKENS, TOPK), 1.5, 6.0, ((0, 8),), jnp.float32)
    gate_weight = bell_draw(key_of[5], (EXPERTS, MODEL_DIM, FF), MODEL_DIM ** -0.5, 0.125, ((0, 8), (2, 4)))
    up_weight = bell_draw(key_of[6], (EXPERTS, MODEL_DIM, FF), MODEL_DIM ** -0.5, 0.125, ((0, 8), (2, 4)))
    down_matrix = bell_draw(key_of[7], (EXPERTS, FF, MODEL_DIM), FF ** -0.5, 0.3125, ((0, 8), (1, 4)))
    return {"tokens": tokens, "norm_gain": norm_gain, "routes": routes, "group_prob": group_prob, "expert_logits": expert_logits, "gate_weight": gate_weight, "up_weight": up_weight, "down_matrix": down_matrix}


def reference(tokens, norm_gain, routes, group_prob, expert_logits, gate_weight, up_weight, down_matrix):
    values = tokens.astype(jnp.float32)
    normed = (values * lax.rsqrt(lax.optimization_barrier(jnp.mean(values * values, -1, keepdims=True)) + 1e-06) * norm_gain).astype(jnp.bfloat16)
    weights = group_prob[:, None] * jax.nn.softmax(expert_logits.astype(jnp.float32), axis=-1)
    flat_ids = routes.reshape(-1)
    flat_weights = weights.reshape(-1)
    upper_limit = N_EP * CAP
    slice_width = FF // N_TP

    def visit(total, expert_index):
        hits = flat_ids == expert_index
        found = jnp.nonzero(hits, size=upper_limit, fill_value=0)[0].astype(jnp.int32)
        usable = jnp.arange(upper_limit, dtype=jnp.int32) < jnp.sum(hits.astype(jnp.int32))
        owners = (found // TOPK).astype(jnp.int32)
        inputs = normed[owners]
        gate_proj = jnp.dot(inputs, gate_weight[expert_index], preferred_element_type=jnp.float32)
        up_proj = jnp.dot(inputs, up_weight[expert_index], preferred_element_type=jnp.float32)
        hidden_state = (jax.nn.silu(gate_proj) * up_proj).astype(jnp.bfloat16)
        block_list = jnp.einsum('lzn,znx->zlx', hidden_state.reshape(upper_limit, N_TP, slice_width).astype(jnp.float32), down_matrix[expert_index].reshape(N_TP, slice_width, MODEL_DIM).astype(jnp.float32)).astype(jnp.bfloat16)
        expert_out = lax.optimization_barrier(jnp.sum(block_list.astype(jnp.float32), 0)).astype(jnp.bfloat16)
        scale = jnp.where(usable, flat_weights[found], jnp.zeros((), jnp.float32))
        total = total.at[owners].add(expert_out.astype(jnp.float32) * scale[:, None])
        return (total, None)
    total, _ = lax.scan(visit, jnp.zeros((TOKENS, MODEL_DIM), jnp.float32), jnp.arange(EXPERTS, dtype=jnp.int32))
    return total.astype(jnp.bfloat16)
```

```python
import functools

import jax
import jax.numpy as jnp
from jax import lax
from jax.experimental import pallas as pl
from jax.experimental.pallas import tpu as pltpu
from jax.sharding import PartitionSpec as P


def hidden_part(buffer, gate_weight, up_weight):
    local_count = gate_weight.shape[0]
    grouped = buffer.reshape(
        buffer.shape[0] // local_count, local_count, buffer.shape[1], buffer.shape[2]
    )
    gate_proj = jnp.einsum(
        "sknd,kdf->sknf", grouped, gate_weight, preferred_element_type=jnp.float32
    )
    up_proj = jnp.einsum("sknd,kdf->sknf", grouped, up_weight, preferred_element_type=jnp.float32)
    hidden_state = (jax.nn.silu(gate_proj) * up_proj).astype(jnp.bfloat16)
    return hidden_state.reshape(buffer.shape[0], buffer.shape[1], hidden_state.shape[3])


def down_blocks(hidden_full, down_cols, block_count):
    local_count = down_cols.shape[0]
    width = hidden_full.shape[2] // block_count
    grouped = hidden_full.reshape(
        hidden_full.shape[0] // local_count, local_count, hidden_full.shape[1], block_count, width
    )
    columns = down_cols.reshape(local_count, block_count, width, down_cols.shape[2])
    block_list = jnp.einsum(
        "sknrf,krfd->sknrd", grouped, columns, preferred_element_type=jnp.float32
    ).astype(jnp.bfloat16)
    summed = jnp.sum(block_list.astype(jnp.float32), 3).astype(jnp.bfloat16)
    return summed.reshape(hidden_full.shape[0], hidden_full.shape[1], down_cols.shape[2])


def body(tokens, norm_gain, routes, group_prob, expert_logits, gate_weight, up_weight, down_matrix):
    tok_rows, model_width = tokens.shape
    top_count = routes.shape[1]
    experts = gate_weight.shape[0] * lax.axis_size("ep")
    capacity = 3 * top_count * tok_rows // (2 * experts)
    block_count = lax.axis_size("tp")
    down_cols = lax.all_to_all(down_matrix, "tp", split_axis=2, concat_axis=1, tiled=True)
    values = tokens.astype(jnp.float32)
    normed = (
        values * lax.rsqrt(jnp.mean(values * values, -1, keepdims=True) + 1e-06) * norm_gain
    ).astype(jnp.bfloat16)
    flat_ids = routes.reshape(-1)
    onehot = (flat_ids[:, None] == jnp.arange(experts, dtype=jnp.int32)[None, :]).astype(jnp.int32)
    earlier = jnp.cumsum(onehot, 0) - onehot
    slot_index = jnp.sum(earlier * onehot, 1)
    target = flat_ids * capacity + slot_index
    owners = jnp.arange(tok_rows * top_count, dtype=jnp.int32) // top_count
    outgoing = (
        jnp.zeros((experts * capacity, model_width), jnp.bfloat16).at[target].set(normed[owners])
    )
    outgoing = outgoing.reshape(experts, capacity, model_width)
    hidden_state = hidden_part(
        lax.all_to_all(outgoing, "ep", split_axis=0, concat_axis=0, tiled=True),
        gate_weight,
        up_weight,
    )
    hidden_full = lax.all_gather(hidden_state, "tp", axis=2, tiled=True)
    summed = down_blocks(hidden_full, down_cols, block_count)
    returned = lax.all_to_all(summed, "ep", split_axis=0, concat_axis=0, tiled=True)
    flat_back = returned.reshape(experts * capacity, returned.shape[2])
    weights = group_prob[:, None] * jax.nn.softmax(expert_logits, axis=-1)
    picked = flat_back[target].reshape(tok_rows, top_count, flat_back.shape[1]).astype(jnp.float32)
    combined = jnp.sum(picked * weights[:, :, None], 1).astype(jnp.bfloat16)
    return combined


MESH = pl.DeviceIdType.MESH
F32, BF16 = jnp.float32, jnp.bfloat16


def round_up(value, step):
    return -(-value // step) * step


def toggled(index, mask):
    bit = 1
    result = index
    while bit <= mask:
        if mask & bit:
            result = result + bit * (1 - 2 * ((index // bit) % 2))
        bit *= 2
    return result


def expert_kernel(
    n_ep, n_tp, capacity, width,
    tokens_ref, gain_ref, routes_ref, prob_ref, logits_ref, gate_ref, up_ref, down_ref,
    out_ref,
    normed, select, weigh, outgoing, arrived, gate_up, down_cols, hidden, result, returned,
    send_disp, recv_disp, send_core, recv_core, send_side, recv_side, send_relay, recv_relay,
    send_down, recv_down, send_hid, recv_hid, send_back, recv_back,
):
    rows, model = tokens_ref.shape
    quarter = model // n_tp
    fpad = gate_up.shape[1] // 2
    n_hi = n_tp // 2
    slots = n_ep * capacity
    e = lax.axis_index("ep")
    t = lax.axis_index("tp")
    partner = t + 1 - 2 * (t % 2)

    def over(index, h):
        return (index + 2 * h) % n_tp

    def back(index, h):
        return (index + n_tp - 2 * h) % n_tp

    barrier = pltpu.get_barrier_semaphore()
    for r in range(1, n_ep):
        pl.semaphore_signal(barrier, inc=1, device_id={"ep": toggled(e, r), "tp": t}, device_id_type=MESH)
    for j in range(1, n_tp):
        pl.semaphore_signal(barrier, inc=1, device_id={"ep": e, "tp": (t + j) % n_tp}, device_id_type=MESH)

    routes = routes_ref[...]
    first, second = routes[:, 0:1], routes[:, 1:2]
    lanes = round_up(n_ep, 128)
    expert_lane = lax.broadcasted_iota(jnp.int32, (rows, lanes), 1)
    hit0 = (expert_lane == first).astype(F32)
    hit1 = (expert_lane == second).astype(F32)
    lower = (
        lax.broadcasted_iota(jnp.int32, (rows, rows), 1) < lax.broadcasted_iota(jnp.int32, (rows, rows), 0)
    ).astype(F32).astype(BF16)
    earlier = jnp.dot(lower, (hit0 + hit1).astype(BF16), preferred_element_type=F32)
    slot0 = jnp.sum(earlier * hit0, 1, keepdims=True)
    slot1 = jnp.sum(earlier * hit1, 1, keepdims=True)
    place0 = first * capacity + slot0.astype(jnp.int32)
    place1 = second * capacity + slot1.astype(jnp.int32)
    slot_lane = lax.broadcasted_iota(jnp.int32, (rows, slots), 1)
    at0, at1 = slot_lane == place0, slot_lane == place1
    named = at0.astype(F32) + at1.astype(F32)
    select[...] = named.T.astype(BF16)

    values = tokens_ref[...].astype(F32)
    scale = lax.rsqrt(jnp.mean(values * values, -1, keepdims=True) + 1e-06)
    normed[...] = (values * scale * gain_ref[...]).astype(BF16)

    mine = normed[:, pl.ds(pl.multiple_of(t * quarter, quarter), quarter)]
    packed = jnp.dot(select[...], mine, preferred_element_type=F32).astype(BF16)
    outgoing[...] = packed.reshape(n_ep, capacity, quarter)

    pl.semaphore_wait(barrier, n_ep - 1 + n_tp - 1)

    def disp(r):
        peer = toggled(e, r)
        return pltpu.make_async_remote_copy(
            src_ref=outgoing.at[peer], dst_ref=arrived.at[r, t], send_sem=send_disp.at[r], recv_sem=recv_disp.at[r],
            device_id={"ep": peer, "tp": t}, device_id_type=MESH)

    def core(r):
        return pltpu.make_async_remote_copy(
            src_ref=arrived.at[r, t], dst_ref=arrived.at[r, t], send_sem=send_core.at[r], recv_sem=recv_core.at[r],
            device_id={"ep": e, "tp": partner}, device_id_type=MESH)

    def side(r, h):
        return pltpu.make_async_remote_copy(
            src_ref=arrived.at[r, t], dst_ref=arrived.at[r, t], send_sem=send_side.at[r, h], recv_sem=recv_side.at[r, h],
            device_id={"ep": e, "tp": over(t, h)}, device_id_type=MESH)

    def relay(r, h):
        origin = back(t, h)
        return pltpu.make_async_remote_copy(
            src_ref=arrived.at[r, origin], dst_ref=arrived.at[r, origin],
            send_sem=send_relay.at[r, h], recv_sem=recv_relay.at[r, h],
            device_id={"ep": e, "tp": partner}, device_id_type=MESH)

    def down(j):
        peer = (t + j) % n_tp
        return pltpu.make_async_remote_copy(
            src_ref=down_ref.at[:, pl.ds(pl.multiple_of(peer * quarter, quarter), quarter)],
            dst_ref=down_cols.at[t, pl.ds(0, width)], send_sem=send_down.at[j], recv_sem=recv_down.at[j],
            device_id={"ep": e, "tp": peer}, device_id_type=MESH)

    def hid(r, j):
        return pltpu.make_async_remote_copy(
            src_ref=hidden.at[r, t], dst_ref=hidden.at[r, t], send_sem=send_hid.at[r, j], recv_sem=recv_hid.at[r, j],
            device_id={"ep": e, "tp": (t + j) % n_tp}, device_id_type=MESH)

    def home(r):
        return pltpu.make_async_remote_copy(
            src_ref=result.at[r], dst_ref=returned.at[e], send_sem=send_back.at[r], recv_sem=recv_back.at[r],
            device_id={"ep": toggled(e, r), "tp": t}, device_id_type=MESH)

    def landed(ref, sem):
        pltpu.make_async_copy(ref, ref, sem).wait()

    for r in ORDER(n_ep):
        disp(r).start()
    for j in range(1, n_tp):
        down(j).start()

    gate_up[...] = jnp.zeros_like(gate_up)
    gate_up[:, 0:width] = gate_ref[...]
    gate_up[:, fpad:fpad + width] = up_ref[...]
    if fpad > width:
        down_cols[:, width:fpad] = jnp.zeros((n_tp, fpad - width, quarter), BF16)
    down_cols[t, 0:width] = down_ref[:, pl.ds(pl.multiple_of(t * quarter, quarter), quarter)]

    logits = logits_ref[...]
    logit0, logit1 = logits[:, 0:1], logits[:, 1:2]
    top = jnp.maximum(logit0, logit1)
    exp0, exp1 = jnp.exp(logit0 - top), jnp.exp(logit1 - top)
    diagonal = lax.broadcasted_iota(jnp.int32, (rows, rows), 0) == lax.broadcasted_iota(jnp.int32, (rows, rows), 1)
    prob = jnp.sum(jnp.where(diagonal, prob_ref[...], 0.0), 1, keepdims=True)
    share = prob / (exp0 + exp1)
    weight = jnp.where(at0, share * exp0, 0.0) + jnp.where(at1, share * exp1, 0.0)
    high = weight.astype(BF16)
    weigh[0] = high
    weigh[1] = (weight - high.astype(F32)).astype(BF16)

    def stage_a(r):
        if r:
            landed(arrived.at[r, t], recv_disp.at[r])
            for h in range(1, n_hi):
                side(r, h).start()
            core(r).start()

    def stage_b(r):
        if r:
            for h in range(1, n_hi):
                landed(arrived.at[r, back(t, h)], recv_side.at[r, h])
                relay(r, h).start()

    def stage_c(r):
        if r:
            landed(arrived.at[r, partner], recv_core.at[r])
            for h in range(1, n_hi):
                landed(arrived.at[r, back(partner, h)], recv_relay.at[r, h])
            acc = jnp.zeros((capacity, 2 * fpad), F32)
            for q in range(n_tp):
                acc = acc + jnp.dot(arrived[r, q], gate_up[q * quarter:(q + 1) * quarter], preferred_element_type=F32)
        else:
            own = select[pl.ds(pl.multiple_of(e * capacity, capacity), capacity)]
            block = jnp.dot(own, normed[...], preferred_element_type=F32).astype(BF16)
            acc = jnp.dot(block, gate_up[...], preferred_element_type=F32)
        gate, up = acc[:, :fpad], acc[:, fpad:]
        hidden[r, t] = (gate / (1.0 + jnp.exp(-gate)) * up).astype(BF16)
        for j in range(1, n_tp):
            hid(r, j).start()

    def stage_d(r, first_time):
        if first_time:
            for j in range(1, n_tp):
                landed(down_cols.at[(t + n_tp - j) % n_tp, pl.ds(0, width)], recv_down.at[j])
        for j in range(1, n_tp):
            landed(hidden.at[r, (t + n_tp - j) % n_tp], recv_hid.at[r, j])
        acc = jnp.zeros((capacity, quarter), F32)
        for q in range(n_tp):
            acc = acc + jnp.dot(hidden[r, q], down_cols[q], preferred_element_type=F32)
        if r:
            result[r] = acc.astype(BF16)
            home(r).start()
        else:
            returned[e] = acc.astype(BF16)

    order = [0] + ORDER(n_ep)
    count = len(order)
    LAG_B, LAG_C, LAG_D = 1, 2, 3
    for step in range(count + LAG_D):
        if step < count:
            stage_a(order[step])
        if 0 <= step - LAG_B < count:
            stage_b(order[step - LAG_B])
        if 0 <= step - LAG_C < count:
            stage_c(order[step - LAG_C])
        if 0 <= step - LAG_D < count:
            stage_d(order[step - LAG_D], step == LAG_D)

    for r in ORDER(n_ep):
        landed(returned.at[toggled(e, r)], recv_back.at[r])
    back_rows = returned[...].reshape(slots, quarter)
    total = jnp.dot(weigh[0], back_rows, preferred_element_type=F32)
    total = total + jnp.dot(weigh[1], back_rows, preferred_element_type=F32)
    out_ref[...] = total.astype(BF16)

    for r in range(1, n_ep):
        disp(r).wait_send()
        core(r).wait_send()
        home(r).wait_send()
        for h in range(1, n_hi):
            side(r, h).wait_send()
            relay(r, h).wait_send()
    for j in range(1, n_tp):
        down(j).wait_send()
        for r in range(n_ep):
            hid(r, j).wait_send()


def ORDER(n_ep):
    return list(range(n_ep - 1, 0, -1))


def fused_body(tokens, norm_gain, routes, group_prob, expert_logits, gate_weight, up_weight, down_matrix):
    n_ep, n_tp = lax.axis_size("ep"), lax.axis_size("tp")
    rows, model = tokens.shape
    capacity = 3 * routes.shape[1] * rows // (2 * n_ep)
    width = gate_weight.shape[2]
    fpad = round_up(width, 128)
    quarter = model // n_tp
    n_hi = n_tp // 2
    sem = pltpu.SemaphoreType.DMA
    vmem = pl.BlockSpec(memory_space=pltpu.VMEM)
    return pl.pallas_call(
        functools.partial(expert_kernel, n_ep, n_tp, capacity, width),
        out_shape=jax.ShapeDtypeStruct((rows, quarter), BF16),
        in_specs=[vmem] * 8,
        out_specs=vmem,
        scratch_shapes=[
            pltpu.VMEM((rows, model), BF16),
            pltpu.VMEM((n_ep * capacity, rows), BF16),
            pltpu.VMEM((2, rows, n_ep * capacity), BF16),
            pltpu.VMEM((n_ep, capacity, quarter), BF16),
            pltpu.VMEM((n_ep, n_tp, capacity, quarter), BF16),
            pltpu.VMEM((model, 2 * fpad), BF16),
            pltpu.VMEM((n_tp, fpad, quarter), BF16),
            pltpu.VMEM((n_ep, n_tp, capacity, fpad), BF16),
            pltpu.VMEM((n_ep, capacity, quarter), BF16),
            pltpu.VMEM((n_ep, capacity, quarter), BF16),
            sem((n_ep,)), sem((n_ep,)),
            sem((n_ep,)), sem((n_ep,)),
            sem((n_ep, n_hi)), sem((n_ep, n_hi)),
            sem((n_ep, n_hi)), sem((n_ep, n_hi)),
            sem((n_tp,)), sem((n_tp,)),
            sem((n_ep, n_tp)), sem((n_ep, n_tp)),
            sem((n_ep,)), sem((n_ep,)),
        ],
        compiler_params=pltpu.CompilerParams(collective_id=0, has_side_effects=True),
    )(
        tokens, norm_gain.reshape(1, model), routes, group_prob.reshape(1, rows), expert_logits,
        gate_weight.reshape(model, width), up_weight.reshape(model, width), down_matrix.reshape(width, model),
    )


def fits_kernel(n_ep, n_tp, rows, experts, top, model):
    capacity = 3 * top * rows // (2 * experts)
    return (
        experts == n_ep and top == 2 and n_ep & (n_ep - 1) == 0 and n_ep <= 16 and n_tp % 2 == 0
        and capacity % 16 == 0 and rows % 128 == 0 and model % (128 * n_tp) == 0
    )


def solution(mesh):
    n_ep, n_tp = mesh.shape["ep"], mesh.shape["tp"]

    def chosen(*arrays):
        rows, model = arrays[0].shape
        fits = fits_kernel(n_ep, n_tp, rows, arrays[5].shape[0] * n_ep, arrays[2].shape[1], model)
        return (fused_body if fits else body)(*arrays)

    return jax.shard_map(
        chosen,
        mesh=mesh,
        in_specs=(
            P("ep", None),
            P(),
            P("ep", None),
            P("ep"),
            P("ep", None),
            P("ep", None, "tp"),
            P("ep", None, "tp"),
            P("ep", "tp", None),
        ),
        out_specs=P("ep", "tp"),
        check_vma=False,
    )
```

```python
import functools

import jax
import jax.numpy as jnp
from jax import lax
from jax.experimental import pallas as pl
from jax.experimental.pallas import tpu as pltpu
from jax.sharding import PartitionSpec as P


def hidden_part(buffer, gate_weight, up_weight):
    local_count = gate_weight.shape[0]
    grouped = buffer.reshape(
        buffer.shape[0] // local_count, local_count, buffer.shape[1], buffer.shape[2]
    )
    gate_proj = jnp.einsum(
        "sknd,kdf->sknf", grouped, gate_weight, preferred_element_type=jnp.float32
    )
    up_proj = jnp.einsum("sknd,kdf->sknf", grouped, up_weight, preferred_element_type=jnp.float32)
    hidden_state = (jax.nn.silu(gate_proj) * up_proj).astype(jnp.bfloat16)
    return hidden_state.reshape(buffer.shape[0], buffer.shape[1], hidden_state.shape[3])


def down_blocks(hidden_full, down_cols, block_count):
    local_count = down_cols.shape[0]
    width = hidden_full.shape[2] // block_count
    grouped = hidden_full.reshape(
        hidden_full.shape[0] // local_count, local_count, hidden_full.shape[1], block_count, width
    )
    columns = down_cols.reshape(local_count, block_count, width, down_cols.shape[2])
    block_list = jnp.einsum(
        "sknrf,krfd->sknrd", grouped, columns, preferred_element_type=jnp.float32
    ).astype(jnp.bfloat16)
    summed = jnp.sum(block_list.astype(jnp.float32), 3).astype(jnp.bfloat16)
    return summed.reshape(hidden_full.shape[0], hidden_full.shape[1], down_cols.shape[2])


def body(tokens, norm_gain, routes, group_prob, expert_logits, gate_weight, up_weight, down_matrix):
    tok_rows, model_width = tokens.shape
    top_count = routes.shape[1]
    experts = gate_weight.shape[0] * lax.axis_size("ep")
    capacity = 3 * top_count * tok_rows // (2 * experts)
    block_count = lax.axis_size("tp")
    down_cols = lax.all_to_all(down_matrix, "tp", split_axis=2, concat_axis=1, tiled=True)
    values = tokens.astype(jnp.float32)
    normed = (
        values * lax.rsqrt(jnp.mean(values * values, -1, keepdims=True) + 1e-06) * norm_gain
    ).astype(jnp.bfloat16)
    flat_ids = routes.reshape(-1)
    onehot = (flat_ids[:, None] == jnp.arange(experts, dtype=jnp.int32)[None, :]).astype(jnp.int32)
    earlier = jnp.cumsum(onehot, 0) - onehot
    slot_index = jnp.sum(earlier * onehot, 1)
    target = flat_ids * capacity + slot_index
    owners = jnp.arange(tok_rows * top_count, dtype=jnp.int32) // top_count
    outgoing = (
        jnp.zeros((experts * capacity, model_width), jnp.bfloat16).at[target].set(normed[owners])
    )
    outgoing = outgoing.reshape(experts, capacity, model_width)
    hidden_state = hidden_part(
        lax.all_to_all(outgoing, "ep", split_axis=0, concat_axis=0, tiled=True),
        gate_weight,
        up_weight,
    )
    hidden_full = lax.all_gather(hidden_state, "tp", axis=2, tiled=True)
    summed = down_blocks(hidden_full, down_cols, block_count)
    returned = lax.all_to_all(summed, "ep", split_axis=0, concat_axis=0, tiled=True)
    flat_back = returned.reshape(experts * capacity, returned.shape[2])
    weights = group_prob[:, None] * jax.nn.softmax(expert_logits, axis=-1)
    picked = flat_back[target].reshape(tok_rows, top_count, flat_back.shape[1]).astype(jnp.float32)
    combined = jnp.sum(picked * weights[:, :, None], 1).astype(jnp.bfloat16)
    return combined


MESH = pl.DeviceIdType.MESH
F32, BF16 = jnp.float32, jnp.bfloat16


def round_up(value, step):
    return -(-value // step) * step


def toggled(index, mask):
    bit = 1
    result = index
    while bit <= mask:
        if mask & bit:
            result = result + bit * (1 - 2 * ((index // bit) % 2))
        bit *= 2
    return result


def expert_kernel(
    n_ep, n_tp, capacity, width,
    tokens_hbm, gain_hbm, routes_hbm, prob_hbm, logits_hbm, gate_ref, up_ref, down_ref,
    out_ref,
    tokens_ref, gain_ref, routes_ref, prob_ref, logits_ref, load_sem, normed, select, weigh, outgoing, arrived, gate_up, down_cols, hidden, result, returned,
    send_disp, recv_disp, send_core, recv_core, send_side, recv_side, send_relay, recv_relay,
    send_down, recv_down, send_hid, recv_hid, send_back, recv_back,
):
    loads = [
        pltpu.make_async_copy(source, target, load_sem.at[i])
        for i, (source, target) in enumerate((
            (routes_hbm, routes_ref), (tokens_hbm, tokens_ref), (gain_hbm, gain_ref),
            (prob_hbm, prob_ref), (logits_hbm, logits_ref),
        ))
    ]
    for load in loads:
        load.start()
    rows, model = tokens_ref.shape
    quarter = model // n_tp
    fpad = gate_up.shape[0] // 2
    n_hi = n_tp // 2
    slots = n_ep * capacity
    e = lax.axis_index("ep")
    t = lax.axis_index("tp")
    partner = t + 1 - 2 * (t % 2)

    def over(index, h):
        return (index + 2 * h) % n_tp

    def back(index, h):
        return (index + n_tp - 2 * h) % n_tp

    barrier = pltpu.get_barrier_semaphore()
    for r in range(1, n_ep):
        pl.semaphore_signal(barrier, inc=1, device_id={"ep": toggled(e, r), "tp": t}, device_id_type=MESH)
    for j in range(1, n_tp):
        pl.semaphore_signal(barrier, inc=1, device_id={"ep": e, "tp": (t + j) % n_tp}, device_id_type=MESH)

    fetch_gate = pltpu.make_async_copy(gate_ref, gate_up.at[pl.ds(0, width)], load_sem.at[5])
    fetch_up = pltpu.make_async_copy(up_ref, gate_up.at[pl.ds(fpad, width)], load_sem.at[6])
    fetch_down = pltpu.make_async_copy(
        down_ref.at[:, pl.ds(pl.multiple_of(t * quarter, quarter), quarter)],
        down_cols.at[t, pl.ds(0, width)], load_sem.at[7])
    fetches = [fetch_gate, fetch_up, fetch_down]
    for fetch in fetches:
        fetch.start()
    for load in loads:
        load.wait()

    first, second = routes_ref[0:1, :], routes_ref[1:2, :]
    lanes = round_up(n_ep, 16)
    expert_row = lax.broadcasted_iota(jnp.int32, (lanes, rows), 0)
    hit0 = (expert_row == first).astype(F32)
    hit1 = (expert_row == second).astype(F32)
    before = (
        lax.broadcasted_iota(jnp.int32, (rows, rows), 0) < lax.broadcasted_iota(jnp.int32, (rows, rows), 1)
    ).astype(F32).astype(BF16)
    earlier = jnp.dot((hit0 + hit1).astype(BF16), before, preferred_element_type=F32)
    slot0 = jnp.sum(earlier * hit0, 0, keepdims=True)
    slot1 = jnp.sum(earlier * hit1, 0, keepdims=True)
    place0 = first * capacity + slot0.astype(jnp.int32)
    place1 = second * capacity + slot1.astype(jnp.int32)
    slot_row = lax.broadcasted_iota(jnp.int32, (slots, rows), 0)
    at0, at1 = slot_row == place0, slot_row == place1
    select[...] = (at0.astype(F32) + at1.astype(F32)).astype(BF16)

    values = tokens_ref[...].astype(F32)
    scale = lax.rsqrt(jnp.mean(values * values, -1, keepdims=True) + 1e-06)
    normed[...] = (values * scale * gain_ref[...]).astype(BF16)

    for h in range(n_hi):
        part = normed[:, pl.ds(pl.multiple_of(back(t, h) * quarter, quarter), quarter)]
        packed = jnp.dot(select[...], part, preferred_element_type=F32).astype(BF16)
        outgoing[h] = packed.reshape(n_ep, capacity, quarter)

    pl.semaphore_wait(barrier, n_ep - 1 + n_tp - 1)

    def disp(r, h=0):
        peer = toggled(e, r)
        origin = back(t, h)
        return pltpu.make_async_remote_copy(
            src_ref=outgoing.at[h, peer], dst_ref=arrived.at[r, origin],
            send_sem=send_disp.at[r, h], recv_sem=recv_disp.at[r, h],
            device_id={"ep": peer, "tp": t}, device_id_type=MESH)

    def core(r):
        return pltpu.make_async_remote_copy(
            src_ref=arrived.at[r, t], dst_ref=arrived.at[r, t], send_sem=send_core.at[r], recv_sem=recv_core.at[r],
            device_id={"ep": e, "tp": partner}, device_id_type=MESH)

    def side(r, h):
        return pltpu.make_async_remote_copy(
            src_ref=arrived.at[r, t], dst_ref=arrived.at[r, t], send_sem=send_side.at[r, h], recv_sem=recv_side.at[r, h],
            device_id={"ep": e, "tp": over(t, h)}, device_id_type=MESH)

    def relay(r, h):
        origin = back(t, h)
        return pltpu.make_async_remote_copy(
            src_ref=arrived.at[r, origin], dst_ref=arrived.at[r, origin],
            send_sem=send_relay.at[r, h], recv_sem=recv_relay.at[r, h],
            device_id={"ep": e, "tp": partner}, device_id_type=MESH)

    def down(j):
        peer = (t + j) % n_tp
        return pltpu.make_async_remote_copy(
            src_ref=down_ref.at[:, pl.ds(pl.multiple_of(peer * quarter, quarter), quarter)],
            dst_ref=down_cols.at[t, pl.ds(0, width)], send_sem=send_down.at[j], recv_sem=recv_down.at[j],
            device_id={"ep": e, "tp": peer}, device_id_type=MESH)

    def hid(p, j):
        return pltpu.make_async_remote_copy(
            src_ref=hidden.at[p, t], dst_ref=hidden.at[p, t], send_sem=send_hid.at[p, j], recv_sem=recv_hid.at[p, j],
            device_id={"ep": e, "tp": (t + j) % n_tp}, device_id_type=MESH)

    def home(r):
        return pltpu.make_async_remote_copy(
            src_ref=result.at[r], dst_ref=returned.at[e], send_sem=send_back.at[r], recv_sem=recv_back.at[r],
            device_id={"ep": toggled(e, r), "tp": t}, device_id_type=MESH)

    def landed(ref, sem):
        pltpu.make_async_copy(ref, ref, sem).wait()

    near = range(1, n_ep // 2)
    far = range(max(1, n_ep // 2), n_ep)
    for r in near:
        for h in range(n_hi):
            disp(r, h).start()
    for r in far:
        disp(r).start()
    for j in range(1, n_tp):
        down(j).start()

    if fpad > width:
        gate_up[width:fpad] = jnp.zeros((fpad - width, model), BF16)
        gate_up[fpad + width:] = jnp.zeros((fpad - width, model), BF16)
        down_cols[:, width:fpad] = jnp.zeros((n_tp, fpad - width, quarter), BF16)

    logit0, logit1 = logits_ref[0:1, :], logits_ref[1:2, :]
    top = jnp.maximum(logit0, logit1)
    exp0, exp1 = jnp.exp(logit0 - top), jnp.exp(logit1 - top)
    share = prob_ref[...] / (exp0 + exp1)
    weight = (jnp.where(at0, share * exp0, 0.0) + jnp.where(at1, share * exp1, 0.0)).T
    high = weight.astype(BF16)
    weigh[0] = high
    weigh[1] = (weight - high.astype(F32)).astype(BF16)

    def product(left, right):
        return lax.dot_general(left, right, (((1,), (1,)), ((), ())), preferred_element_type=F32)

    def take(r):
        landed(arrived.at[r, t], recv_disp.at[r, 0])
        if r in far:
            for h in range(1, n_hi):
                side(r, h).start()
        core(r).start()
        if r in near:
            for h in range(1, n_hi):
                landed(arrived.at[r, back(t, h)], recv_disp.at[r, h])
                relay(r, h).start()

    def pass_on(r):
        for h in range(1, n_hi):
            landed(arrived.at[r, back(t, h)], recv_side.at[r, h])
            relay(r, h).start()

    def expand(p):
        for r in (2 * p, 2 * p + 1):
            if r:
                landed(arrived.at[r, partner], recv_core.at[r])
                for h in range(1, n_hi):
                    landed(arrived.at[r, back(partner, h)], recv_relay.at[r, h])
            else:
                own = select[pl.ds(pl.multiple_of(e * capacity, capacity), capacity)]
                for q in range(n_tp):
                    block = jnp.dot(own, normed[:, q * quarter:(q + 1) * quarter], preferred_element_type=F32)
                    arrived[0, q] = block.astype(BF16)
        acc = jnp.zeros((2 * capacity, 2 * fpad), F32)
        for q in range(n_tp):
            block = arrived[2 * p:2 * p + 2, q].reshape(2 * capacity, quarter)
            acc = acc + product(block, gate_up[:, q * quarter:(q + 1) * quarter])
        gate, up = acc[:, :fpad], acc[:, fpad:]
        hidden[p, t] = (gate / (1.0 + jnp.exp(-gate)) * up).astype(BF16)
        for j in range(1, n_tp):
            hid(p, j).start()

    def contract(p):
        for j in range(1, n_tp):
            landed(hidden.at[p, (t + n_tp - j) % n_tp], recv_hid.at[p, j])
        acc = jnp.zeros((2 * capacity, quarter), F32)
        for q in range(n_tp):
            acc = acc + jnp.dot(hidden[p, q], down_cols[q], preferred_element_type=F32)
        for i in range(2):
            r = 2 * p + i
            block = acc[i * capacity:(i + 1) * capacity].astype(BF16)
            if r:
                result[r] = block
                home(r).start()
            else:
                returned[e] = block

    for fetch in fetches:
        fetch.wait()
    pairs = n_ep // 2
    todo = []
    for p in range(pairs):
        rounds = [r for r in (2 * p, 2 * p + 1) if r]
        todo.append((3 * p, take, rounds))
        todo.append((3 * p + 3, pass_on, [r for r in rounds if r in far]))
        todo.append((3 * p + 4 if rounds[0] in far else 3 * p + 2, expand, [p]))
        todo.append((3 * p + 8 if rounds[0] in far else 3 * p + 6, contract, [p]))
    todo.sort(key=lambda entry: entry[0])
    waited = False
    for _, stage, items in todo:
        if stage is contract and not waited:
            waited = True
            for j in range(1, n_tp):
                landed(down_cols.at[(t + n_tp - j) % n_tp, pl.ds(0, width)], recv_down.at[j])
        for item in items:
            stage(item)

    for r in range(1, n_ep):
        landed(returned.at[toggled(e, r)], recv_back.at[r])
    back_rows = returned[...].reshape(slots, quarter)
    total = jnp.dot(weigh[0], back_rows, preferred_element_type=F32)
    total = total + jnp.dot(weigh[1], back_rows, preferred_element_type=F32)
    out_ref[...] = total.astype(BF16)

    for r in range(1, n_ep):
        disp(r).wait_send()
        core(r).wait_send()
        home(r).wait_send()
        for h in range(1, n_hi):
            if r in near:
                disp(r, h).wait_send()
            else:
                side(r, h).wait_send()
            relay(r, h).wait_send()
    for j in range(1, n_tp):
        down(j).wait_send()
        for p in range(pairs):
            hid(p, j).wait_send()


def fused_body(tokens, norm_gain, routes, group_prob, expert_logits, gate_weight, up_weight, down_matrix):
    n_ep, n_tp = lax.axis_size("ep"), lax.axis_size("tp")
    rows, model = tokens.shape
    capacity = 3 * routes.shape[1] * rows // (2 * n_ep)
    width = gate_weight.shape[2]
    fpad = round_up(width, 128)
    quarter = model // n_tp
    n_hi = n_tp // 2
    sem = pltpu.SemaphoreType.DMA
    vmem = pl.BlockSpec(memory_space=pltpu.VMEM)
    return pl.pallas_call(
        functools.partial(expert_kernel, n_ep, n_tp, capacity, width),
        out_shape=jax.ShapeDtypeStruct((rows, quarter), BF16),
        in_specs=[pl.BlockSpec(memory_space=pl.ANY)] * 8,
        out_specs=vmem,
        scratch_shapes=[
            pltpu.VMEM((rows, model), BF16),
            pltpu.VMEM((1, model), F32),
            pltpu.VMEM((2, rows), jnp.int32),
            pltpu.VMEM((1, rows), F32),
            pltpu.VMEM((2, rows), F32),
            sem((8,)),
            pltpu.VMEM((rows, model), BF16),
            pltpu.VMEM((n_ep * capacity, rows), BF16),
            pltpu.VMEM((2, rows, n_ep * capacity), BF16),
            pltpu.VMEM((n_hi, n_ep, capacity, quarter), BF16),
            pltpu.VMEM((n_ep, n_tp, capacity, quarter), BF16),
            pltpu.VMEM((2 * fpad, model), BF16),
            pltpu.VMEM((n_tp, fpad, quarter), BF16),
            pltpu.VMEM((n_ep // 2, n_tp, 2 * capacity, fpad), BF16),
            pltpu.VMEM((n_ep, capacity, quarter), BF16),
            pltpu.VMEM((n_ep, capacity, quarter), BF16),
            sem((n_ep, n_hi)), sem((n_ep, n_hi)),
            sem((n_ep,)), sem((n_ep,)),
            sem((n_ep, n_hi)), sem((n_ep, n_hi)),
            sem((n_ep, n_hi)), sem((n_ep, n_hi)),
            sem((n_tp,)), sem((n_tp,)),
            sem((n_ep, n_tp)), sem((n_ep, n_tp)),
            sem((n_ep,)), sem((n_ep,)),
        ],
        compiler_params=pltpu.CompilerParams(collective_id=0, has_side_effects=True),
    )(
        tokens, norm_gain.reshape(1, model), routes.T, group_prob.reshape(1, rows), expert_logits.T,
        gate_weight.reshape(model, width).T, up_weight.reshape(model, width).T, down_matrix.reshape(width, model),
    )


def fits_kernel(n_ep, n_tp, rows, experts, top, model):
    capacity = 3 * top * rows // (2 * experts)
    return (
        experts == n_ep and top == 2 and n_ep & (n_ep - 1) == 0 and n_ep <= 16 and n_tp % 2 == 0
        and capacity % 16 == 0 and rows % 128 == 0 and model % (128 * n_tp) == 0
    )


def solution(mesh):
    n_ep, n_tp = mesh.shape["ep"], mesh.shape["tp"]

    def chosen(*arrays):
        rows, model = arrays[0].shape
        fits = fits_kernel(n_ep, n_tp, rows, arrays[5].shape[0] * n_ep, arrays[2].shape[1], model)
        return (fused_body if fits else body)(*arrays)

    return jax.shard_map(
        chosen,
        mesh=mesh,
        in_specs=(
            P("ep", None),
            P(),
            P("ep", None),
            P("ep"),
            P("ep", None),
            P("ep", None, "tp"),
            P("ep", None, "tp"),
            P("ep", "tp", None),
        ),
        out_specs=P("ep", "tp"),
        check_vma=False,
    )
```
